128 devices in a mesh: fs: 16 (over z, x), tp: 8 (over y, core).
Axes of the slice: x: 4, y: 4, z: 4, core: 2. Of those that a mesh axis runs over, the one named last changes fastest.
Arguments:
- normed_input: bfloat16 [32768, 2048], P('fs'), may hold values from -6 to 6
- forget_cot: bfloat16 [32768, 2048], P('fs', 'tp'), may hold values from -6 to 6
- value_cot: bfloat16 [32768, 2048], P('fs', 'tp'), may hold values from -6 to 6
- gated_output: bfloat16 [32768, 2048], P('fs', 'tp'), may hold values from -6 to 6
- output_cot: bfloat16 [32768, 2048], P('fs'), may hold values from -6 to 6
- forget_weight: float32 [2048, 2048], P('fs', 'tp'), may hold values from -0.125 to 0.125
- value_weight: float32 [2048, 2048], P('fs', 'tp'), may hold values from -0.125 to 0.125
- out_weight: float32 [2048, 2048], P('tp', 'fs'), may hold values from -0.125 to 0.125
- bases: bfloat16 [3, 2048, 256], replicated, may hold values from -0.125 to 0.125
- first_moment: float32 [256, 3, 2048], P('fs', None, 'tp'), may hold values from -4 to 4
- second_moment: float32 [256, 3, 2048], P('fs', None, 'tp'), may hold values from 0.25 to 4
Outputs:
- new_forget: float32 [2048, 2048], P('fs', 'tp')
- new_value: float32 [2048, 2048], P('fs', 'tp')
- new_out: float32 [2048, 2048], P('tp', 'fs')
- copy_forget: bfloat16 [2048, 2048], P(None, 'tp')
- copy_value: bfloat16 [2048, 2048], P(None, 'tp')
- copy_out: bfloat16 [2048, 2048], P('tp')
- moment_one: float32 [256, 3, 2048], P('fs', None, 'tp')
- moment_two: float32 [256, 3, 2048], P('fs', None, 'tp')
- step_forget: float32 [2048, 2048], P('fs', 'tp')
- step_value: float32 [2048, 2048], P('fs', 'tp')
- step_out: float32 [2048, 2048], P('tp', 'fs')
The draws below stay inside these ranges and needn't reach their ends.
All inputs are finite; a program needn't handle non-finite values.
Results may differ from the reference program's by a relative error of at most 0.0045.
Values may be sent and summed in bfloat16 or wider, within the bound.
No kernel may reach another device: no remote copies, remote signals or barrier semaphores. Data moves between devices by JAX's collectives and lax.ppermute only.
A program may use at most 128 MiB of HBM per device.

```python
import math
import jax
import jax.numpy as jnp
from jax import lax

D = 2048
QK = 2048
V = 2048
RANK = 256
TOKENS = 32768


def draw_first_moment(key, part):
    base = jax.random.normal(key, (RANK, 3, QK), jnp.float32) * 0.5
    return jnp.clip(base, -4.0, 4.0)


def level_of(rng, dims, shards, smallest, top_value):
    gain = 1.0
    for dim, shards_of in shards:
        heights = jax.random.uniform(jax.random.fold_in(jax.random.fold_in(rng, 6), dim), (shards_of,), jnp.float32, smallest / len(shards), top_value / len(shards))
        gain = gain * jnp.repeat(jnp.exp(heights), dims[dim] // shards_of).reshape((-1,) + (1,) * (len(dims) - 1 - dim))
    return gain


def normal_values(rng, extent, spread, reach, shards=(), dtype=jnp.bfloat16):
    values = spread * jax.random.normal(rng, extent, jnp.float32)
    if shards:
        values = values * level_of(rng, extent, shards, -0.22, 0.18)
    return jnp.clip(values, -reach, reach).astype(dtype)


def setup_inputs(seed: int = 0) -> dict:
    arg_keys = jax.random.split(jax.random.key(seed), 12)
    normed_input = normal_values(arg_keys[0], (TOKENS, D), 1.0, 6.0, ((0, 16),))
    forget_cot = normal_values(arg_keys[1], (TOKENS, QK), 1.0, 6.0, ((0, 16), (1, 8)))
    value_cot = normal_values(arg_keys[2], (TOKENS, V), 1.0, 6.0, ((0, 16), (1, 8)))
    gated_output = normal_values(arg_keys[3], (TOKENS, V), 1.0, 6.0, ((0, 16), (1, 8)))
    output_cot = normal_values(arg_keys[4], (TOKENS, D), 1.0, 6.0, ((0, 16),))
    forget_weight = normal_values(arg_keys[5], (D, QK), D ** -0.5, 0.125, ((0, 16), (1, 8)), jnp.float32)
    value_weight = normal_values(arg_keys[6], (D, V), D ** -0.5, 0.125, ((0, 16), (1, 8)), jnp.float32)
    out_weight = normal_values(arg_keys[7], (V, D), V ** -0.5, 0.125, ((0, 8), (1, 16)), jnp.float32)
    bases = normal_values(arg_keys[8], (3, D, RANK), D ** -0.5, 0.125)
    first_moment = draw_first_moment(jax.random.fold_in(arg_keys[11], 71), 0)
    second_moment = jnp.clip(jnp.exp(math.log(4.0) - 2.7725887 * jax.random.uniform(arg_keys[10], (RANK, 3, QK), jnp.float32) ** level_of(arg_keys[10], (RANK, 3, QK), ((0, 16), (2, 8)), -0.2, 0.2)), 0.25, 4.0)
    return {"normed_input": normed_input, "forget_cot": forget_cot, "value_cot": value_cot, "gated_output": gated_output, "output_cot": output_cot, "forget_weight": forget_weight, "value_weight": value_weight, "out_weight": out_weight, "bases": bases, "first_moment": first_moment, "second_moment": second_moment}


def reference(normed_input, forget_cot, value_cot, gated_output, output_cot, forget_weight, value_weight, out_weight, bases, first_moment, second_moment):
    factor = float(TOKENS) ** (-0.5)
    grad_forget = jnp.dot(normed_input.T, forget_cot, preferred_element_type=jnp.float32) * factor
    grad_value = jnp.dot(normed_input.T, value_cot, preferred_element_type=jnp.float32) * factor
    grad_out = jnp.dot(output_cot.T, gated_output, preferred_element_type=jnp.float32) * factor
    grads = jnp.stack([grad_forget, grad_value, grad_out], axis=1)
    basis_full = bases.astype(jnp.float32)
    projected = jnp.einsum('kdr,dkc->rkc', basis_full, grads, precision=lax.Precision.HIGHEST)
    moment_one = 0.9 * first_moment + 0.1 * projected
    moment_two = 0.9 * second_moment + 0.1 * projected * projected
    direction = moment_one / (jnp.sqrt(moment_two) + 1e-08)
    scale = lax.rsqrt(lax.optimization_barrier(jnp.mean(direction * direction, axis=(0, 2))) + 1.0)
    full = jnp.einsum('kdr,rkc->dkc', basis_full, direction, precision=lax.Precision.HIGHEST)
    full = full * scale[None, :, None]
    step_forget = full[:, 0, :]
    step_value = full[:, 1, :]
    step_out = full[:, 2, :].T
    new_forget = forget_weight - 0.01 * step_forget
    new_value = value_weight - 0.01 * step_value
    new_out = out_weight - 0.01 * step_out
    return (new_forget, new_value, new_out, new_forget.astype(jnp.bfloat16), new_value.astype(jnp.bfloat16), new_out.astype(jnp.bfloat16), moment_one, moment_two, step_forget, step_value, step_out)
```

```python
import functools

import jax
import jax.numpy as jnp
from jax import lax
from jax.experimental import pallas as pl
from jax.experimental.pallas import tpu as pltpu
from jax.sharding import Mesh
from jax.sharding import PartitionSpec as P

FS = ("fs_0", "fs_1")
TP = ("tp_0", "tp_1")

NEAR, FAR = 1, 3
STREAMS = (
    (4 * NEAR, 4 * FAR, NEAR, FAR),
    (4 * FAR, 4 * NEAR, FAR, NEAR),
    (NEAR, FAR, 4 * NEAR, 4 * FAR),
    (FAR, NEAR, 4 * FAR, 4 * NEAR),
)
QUARTERS = len(STREAMS)
EARLY = pl.CostEstimate(flops=1 << 34, bytes_accessed=1 << 20, transcendentals=0)
SMALL = pltpu.CompilerParams(vmem_limit_bytes=8 << 20)
LARGE = pltpu.CompilerParams(vmem_limit_bytes=24 << 20)


def fs_of_position(masks, position):
    return functools.reduce(
        lambda a, b: a ^ b, [m for s, m in enumerate(masks) if position >> s & 1], 0
    )


def opening_kernel(out_ref):
    out_ref[...] = jnp.zeros_like(out_ref)


def opening():
    return pl.pallas_call(
        opening_kernel,
        out_shape=jax.ShapeDtypeStruct((8, 128), jnp.float32),
        cost_estimate=EARLY,
        compiler_params=SMALL,
        name="opening",
    )()


def pack_kernel(_, forget_ref, value_ref, out_ref, *packed_refs):
    rows = forget_ref.shape[0] // QUARTERS
    width = out_ref.shape[1]
    tall = out_ref.shape[0] // QUARTERS
    for q, packed in enumerate(packed_refs):
        near = pl.ds(q * rows, rows)
        packed[0, :rows] = forget_ref[near].astype(jnp.bfloat16)
        packed[0, rows : 2 * rows] = value_ref[near].astype(jnp.bfloat16)
        for h in range(tall // rows):
            part = out_ref[pl.ds(q * tall + h * rows, rows)]
            packed[0, 2 * rows :, h * width : (h + 1) * width] = part.astype(jnp.bfloat16)


def pack(opened, *weights):
    rows, columns = weights[0].shape
    shape = jax.ShapeDtypeStruct((1, 3 * rows // QUARTERS, columns), jnp.bfloat16)
    return pl.pallas_call(
        pack_kernel,
        out_shape=(shape,) * QUARTERS,
        cost_estimate=EARLY,
        compiler_params=SMALL,
        name="pack",
    )(opened, *weights)


def reduced_part(x, basis):
    reduced = lax.dot_general(
        basis, x, (((0,), (1,)), ((), ())), preferred_element_type=jnp.float32
    )
    return reduced.astype(jnp.bfloat16)


def projected_part(reduced, cot, factor):
    part = jnp.dot(reduced, cot, preferred_element_type=jnp.float32)
    return (part * factor).astype(jnp.bfloat16)


def moment_kernel(arrived_ref, first_ref, second_ref, one_ref, two_ref, message_ref):
    rows = first_ref.shape[1]
    for k in range(3):
        projected = jnp.sum(arrived_ref[:, k].astype(jnp.float32), axis=0)
        one = 0.9 * first_ref[k] + 0.1 * projected
        two = 0.9 * second_ref[k] + 0.1 * projected * projected
        one_ref[k] = one
        two_ref[k] = two
        direction = (one / (jnp.sqrt(two) + 1e-08)).astype(jnp.bfloat16)
        for i in range(message_ref.shape[0]):
            message_ref[i, k * rows : (k + 1) * rows] = direction


def moments(arrived, first_moment, second_moment):
    _, rows, columns = first_moment.shape
    moment = jax.ShapeDtypeStruct(first_moment.shape, jnp.float32)
    messages = jax.ShapeDtypeStruct((arrived.shape[0], 3 * rows, columns), jnp.bfloat16)
    return pl.pallas_call(
        moment_kernel,
        out_shape=(moment, moment, messages),
        compiler_params=SMALL,
        name="moments",
    )(arrived, first_moment, second_moment)


def square_kernel(arrived_ref, sum_ref):
    rows = arrived_ref.shape[1] // 3
    lane = lax.broadcasted_iota(jnp.int32, sum_ref.shape, 1)
    sums = jnp.zeros(sum_ref.shape, jnp.float32)
    for k in range(3):
        direction = arrived_ref[:, k * rows : (k + 1) * rows].astype(jnp.float32)
        sums = jnp.where(lane == k, jnp.sum(direction * direction), sums)
    sum_ref[...] = sums


def squares(arrived):
    return pl.pallas_call(
        square_kernel,
        out_shape=jax.ShapeDtypeStruct((1, 128), jnp.float32),
        compiler_params=SMALL,
        name="squares",
    )(arrived)


def finish_kernel(entries, me_ref, sums_ref, arrived_ref, base_ref, mine_ref, forget_ref, value_ref, outw_ref, *refs):
    held = [refs[2 * q : 2 * q + 2] for q in range(QUARTERS)]
    (
        new_forget,
        new_value,
        new_out,
        copy_forget,
        copy_value,
        copy_out,
        step_forget,
        step_value,
        step_out,
        dir_ref,
        scale_ref,
    ) = refs[2 * QUARTERS :]
    step = pl.program_id(0)
    owners = arrived_ref.shape[0]
    rank = dir_ref.shape[1]
    rows = rank // owners
    block = mine_ref.shape[1]
    width = outw_ref.shape[1]
    part = block // QUARTERS
    tall = outw_ref.shape[0] // QUARTERS
    me = me_ref[0]
    by_columns = (((1,), (1,)), ((), ()))

    @pl.when(step == 0)
    def _():
        sums = jnp.sum(sums_ref[...], axis=0)
        scale_ref[...] = lax.rsqrt(sums / entries + 1.0)
        for k in range(3):
            direction = arrived_ref[:, k * rows : (k + 1) * rows, :].reshape(rank, -1)
            dir_ref[k] = direction if k < 2 else direction.T
        for k, (old, new, moved) in enumerate(
            ((forget_ref, new_forget, step_forget), (value_ref, new_value, step_value))
        ):
            full = jnp.dot(mine_ref[k], dir_ref[k], preferred_element_type=jnp.float32)
            full = full * scale_ref[0, k]
            moved[...] = full
            new[...] = old[...] - 0.01 * full
        full = lax.dot_general(dir_ref[2], mine_ref[2], by_columns, preferred_element_type=jnp.float32)
        full = full * scale_ref[0, 2]
        step_out[...] = full
        new_out[...] = outw_ref[...] - 0.01 * full

    moves = []
    for k in range(2):
        full = jnp.dot(base_ref[k], dir_ref[k], preferred_element_type=jnp.float32)
        moves.append(full * (0.01 * scale_ref[0, k]))
    full = lax.dot_general(dir_ref[2], base_ref[2], by_columns, preferred_element_type=jnp.float32)
    moves.append(full * (0.01 * scale_ref[0, 2]))
    half = owners // 2
    for j in range(base_ref.shape[1] // block):
        other = me ^ (step * (base_ref.shape[1] // block) + j)
        for q, masks in enumerate(STREAMS):
            position = jnp.int32(0)
            for p in range(owners):
                position = jnp.where(other == fs_of_position(masks, p), p, position)
            early, late = held[q]
            old = jnp.where(position < half, early[position % half], late[position % half])
            old = old.astype(jnp.float32)
            near = slice(j * block + q * part, j * block + (q + 1) * part)
            copy_forget[near] = (old[:part] - moves[0][near]).astype(jnp.bfloat16)
            copy_value[near] = (old[part : 2 * part] - moves[1][near]).astype(jnp.bfloat16)
            for h in range(tall // part):
                down = slice(q * tall + h * part, q * tall + (h + 1) * part)
                across = slice(j * width, (j + 1) * width)
                piece = old[2 * part :, h * width : (h + 1) * width]
                copy_out[down, across] = (piece - moves[2][down, across]).astype(jnp.bfloat16)


def finish(me, sums, arrived, bases, forget_weight, value_weight, out_weight, held, entries, steps=4):
    block, columns = forget_weight.shape
    model, rank = bases.shape[1:]
    tile = model // steps
    whole = lambda a: pl.BlockSpec(a.shape, lambda i, me: (0,) * a.ndim)
    old = (forget_weight, value_weight, out_weight)
    own = [jax.ShapeDtypeStruct(a.shape, jnp.float32) for a in old]
    copies = [jax.ShapeDtypeStruct((model, columns), jnp.bfloat16)] * 2
    copies.append(jax.ShapeDtypeStruct((out_weight.shape[0], model), jnp.bfloat16))
    down = pl.BlockSpec((tile, columns), lambda i, me: (i, 0))
    across = pl.BlockSpec((out_weight.shape[0], tile), lambda i, me: (0, i))
    flat = [a for pair in held for a in pair]
    return pl.pallas_call(
        functools.partial(finish_kernel, entries),
        grid_spec=pltpu.PrefetchScalarGridSpec(
            num_scalar_prefetch=1,
            grid=(steps,),
            in_specs=[
                whole(sums),
                whole(arrived),
                pl.BlockSpec((3, tile, rank), lambda i, me: (0, i, 0)),
                pl.BlockSpec((3, block, rank), lambda i, me: (0, me[0], 0)),
                *map(whole, old),
                *map(whole, flat),
            ],
            out_specs=[
                *map(whole, own),
                down,
                down,
                across,
                *map(whole, own),
            ],
            scratch_shapes=[
                pltpu.VMEM((3, rank, columns), jnp.bfloat16),
                pltpu.VMEM((1, 128), jnp.float32),
            ],
        ),
        out_shape=(*own, *copies, *own),
        compiler_params=LARGE,
        name="finish",
    )(me[None], sums, arrived, bases, bases, *old, *flat)


def swap_all(held, step):
    owners = lax.axis_size(FS)
    received = []
    for masks, value in zip(STREAMS, held):
        pairs = [(i, i ^ masks[step]) for i in range(owners)]
        received.append(lax.ppermute(value, FS, pairs))
    return received


def joined(held, received):
    return [jnp.concatenate(pair) for pair in zip(held, received)]


def on_device(
    normed_input,
    forget_cot,
    value_cot,
    gated_output,
    output_cot,
    forget_weight,
    value_weight,
    out_weight,
    bases,
    first_moment,
    second_moment,
):
    owners = lax.axis_size(FS)
    me = lax.axis_index(FS).astype(jnp.int32)
    factor = float(normed_input.shape[0] * owners) ** (-0.5)
    rank, columns = bases.shape[2], forget_cot.shape[1]
    held = list(pack(opening(), forget_weight, value_weight, out_weight))
    received = swap_all(held, 0)
    inputs = (normed_input, normed_input, output_cot)
    cots = (forget_cot, value_cot, gated_output)
    reduced = [reduced_part(x, bases[k]) for k, x in enumerate(inputs)]
    reduced = lax.optimization_barrier(tuple(reduced))
    parts = [projected_part(r, c, factor) for r, c in zip(reduced, cots)]
    part = jnp.stack([p.reshape(owners, rank // owners, columns) for p in parts], axis=1)
    held = joined(held, received)
    part, *held = lax.optimization_barrier((part, *held))
    arrived = lax.all_to_all(part, FS, split_axis=0, concat_axis=0, tiled=True)
    received = swap_all(held, 1)
    moment_one, moment_two, messages = moments(
        arrived, jnp.moveaxis(first_moment, 1, 0), jnp.moveaxis(second_moment, 1, 0)
    )
    held = joined(held, received)
    messages, *held = lax.optimization_barrier((messages, *held))
    gathered = lax.all_to_all(messages, FS, split_axis=0, concat_axis=0, tiled=True)
    received = swap_all(held, 2)
    sums = squares(gathered)
    held = joined(held, received)
    sums, *held = lax.optimization_barrier((sums, *held))
    received = swap_all(held, 3)
    sums = lax.all_gather(sums, TP, axis=0)
    entries = float(rank * columns * lax.axis_size(TP))
    finished = finish(
        me,
        sums,
        gathered,
        bases,
        forget_weight,
        value_weight,
        out_weight,
        list(zip(held, received)),
        entries,
    )
    moment_one, moment_two = (jnp.moveaxis(m, 0, 1) for m in (moment_one, moment_two))
    return (*finished[:6], moment_one, moment_two, *finished[6:])


def solution(mesh):
    torus = Mesh(mesh.devices.reshape(4, 4, 4, 2), ("fs_0", "fs_1", "tp_0", "tp_1"))
    placed = (
        P(FS, None),
        P(FS, TP),
        P(FS, TP),
        P(FS, TP),
        P(FS, None),
        P(FS, TP),
        P(FS, TP),
        P(TP, FS),
        P(),
        P(FS, None, TP),
        P(FS, None, TP),
    )
    return jax.shard_map(
        on_device,
        mesh=torus,
        in_specs=placed,
        out_specs=(
            P(FS, TP),
            P(FS, TP),
            P(TP, FS),
            P(None, TP),
            P(None, TP),
            P(TP, None),
            P(FS, None, TP),
            P(FS, None, TP),
            P(FS, TP),
            P(FS, TP),
            P(TP, FS),
        ),
        check_vma=False,
    )
```

```python
import functools

import jax
import jax.numpy as jnp
from jax import lax
from jax.experimental import pallas as pl
from jax.experimental.pallas import tpu as pltpu
from jax.sharding import Mesh
from jax.sharding import PartitionSpec as P


FS = ("fs_0", "fs_1")
TP = ("tp_0", "tp_1")

NEAR, FAR = 1, 3
SIDE = 4
TURNS = ((NEAR, FAR), (FAR, NEAR))
EARLY = pl.CostEstimate(flops=1 << 34, bytes_accessed=1 << 20, transcendentals=0)
SMALL = pltpu.CompilerParams(vmem_limit_bytes=8 << 20)
LARGE = pltpu.CompilerParams(vmem_limit_bytes=24 << 20)


def opening_kernel(out_ref):
    out_ref[...] = jnp.zeros_like(out_ref)


def opening():
    return pl.pallas_call(
        opening_kernel,
        out_shape=jax.ShapeDtypeStruct((8, 128), jnp.float32),
        cost_estimate=EARLY,
        compiler_params=SMALL,
        name="opening",
    )()


def pack_kernel(_, forget_ref, value_ref, out_ref, packed_ref):
    rows = forget_ref.shape[0]
    width = out_ref.shape[1]
    packed_ref[0, :rows] = forget_ref[...].astype(jnp.bfloat16)
    packed_ref[0, rows : 2 * rows] = value_ref[...].astype(jnp.bfloat16)
    for h in range(out_ref.shape[0] // rows):
        part = out_ref[pl.ds(h * rows, rows)]
        packed_ref[0, 2 * rows :, h * width : (h + 1) * width] = part.astype(jnp.bfloat16)


def pack(opened, *weights):
    rows, columns = weights[0].shape
    return pl.pallas_call(
        pack_kernel,
        out_shape=jax.ShapeDtypeStruct((1, 3 * rows, columns), jnp.bfloat16),
        cost_estimate=EARLY,
        compiler_params=SMALL,
        name="pack",
    )(opened, *weights)


def reduced_part(x, basis):
    reduced = lax.dot_general(
        basis, x, (((0,), (1,)), ((), ())), preferred_element_type=jnp.float32
    )
    return reduced.astype(jnp.bfloat16)


def projected_part(reduced, cot, factor):
    part = jnp.dot(reduced, cot, preferred_element_type=jnp.float32)
    return (part * factor).astype(jnp.bfloat16)


def moment_kernel(arrived_ref, first_ref, second_ref, one_ref, two_ref, message_ref):
    rows = first_ref.shape[1]
    for k in range(3):
        projected = jnp.sum(arrived_ref[:, k].astype(jnp.float32), axis=0)
        one = 0.9 * first_ref[k] + 0.1 * projected
        two = 0.9 * second_ref[k] + 0.1 * projected * projected
        one_ref[k] = one
        two_ref[k] = two
        direction = (one / (jnp.sqrt(two) + 1e-08)).astype(jnp.bfloat16)
        for i in range(message_ref.shape[0]):
            message_ref[i, k * rows : (k + 1) * rows] = direction


def moments(arrived, first_moment, second_moment):
    _, rows, columns = first_moment.shape
    moment = jax.ShapeDtypeStruct(first_moment.shape, jnp.float32)
    messages = pltpu.HBM((arrived.shape[0], 3 * rows, columns), jnp.bfloat16)
    return pl.pallas_call(
        moment_kernel,
        out_shape=(moment, moment, messages),
        compiler_params=SMALL,
        name="moments",
    )(arrived, first_moment, second_moment)


def square_kernel(arrived_ref, sum_ref):
    rows = arrived_ref.shape[1] // 3
    lane = lax.broadcasted_iota(jnp.int32, sum_ref.shape, 2)
    sums = jnp.zeros(sum_ref.shape, jnp.float32)
    for k in range(3):
        direction = arrived_ref[:, k * rows : (k + 1) * rows].astype(jnp.float32)
        sums = jnp.where(lane == k, jnp.sum(direction * direction), sums)
    sum_ref[...] = sums


def squares(arrived, copies):
    return pl.pallas_call(
        square_kernel,
        out_shape=jax.ShapeDtypeStruct((copies, 1, 128), jnp.float32),
        compiler_params=SMALL,
        name="squares",
    )(arrived)


def finish_kernel(entries, me_ref, sums_ref, arrived_ref, base_ref, mine_ref, forget_ref, value_ref, outw_ref, *refs):
    streams = len(TURNS)
    held = []
    for t in range(streams):
        whole, nearer, even, odd, across = refs[5 * t : 5 * t + 5]
        held.append((whole, nearer, (even, odd), across))
    (
        new_forget,
        new_value,
        new_out,
        copy_forget,
        copy_value,
        copy_out,
        step_forget,
        step_value,
        step_out,
        dir_ref,
        scale_ref,
        old_ref,
    ) = refs[5 * streams :]
    step = pl.program_id(0)
    owners = arrived_ref.shape[0]
    rank = dir_ref.shape[1]
    rows = rank // owners
    block = mine_ref.shape[1]
    width = outw_ref.shape[1]
    me = me_ref[0]
    by_columns = (((1,), (1,)), ((), ()))

    @pl.when(step == 0)
    def _():
        sums = jnp.sum(sums_ref[...], axis=0)
        scale_ref[...] = lax.rsqrt(sums / entries + 1.0)
        for k in range(3):
            direction = arrived_ref[:, k * rows : (k + 1) * rows, :].reshape(rank, -1)
            dir_ref[k] = direction if k < 2 else direction.T
        for k, (old, new, moved) in enumerate(
            ((forget_ref, new_forget, step_forget), (value_ref, new_value, step_value))
        ):
            full = jnp.dot(mine_ref[k], dir_ref[k], preferred_element_type=jnp.float32)
            full = full * scale_ref[0, k]
            moved[...] = full
            new[...] = old[...] - 0.01 * full
        full = lax.dot_general(dir_ref[2], mine_ref[2], by_columns, preferred_element_type=jnp.float32)
        full = full * scale_ref[0, 2]
        step_out[...] = full
        new_out[...] = outw_ref[...] - 0.01 * full

    moves = []
    for k in range(2):
        full = jnp.dot(base_ref[k], dir_ref[k], preferred_element_type=jnp.float32)
        moves.append(full * (0.01 * scale_ref[0, k]))
    full = lax.dot_general(dir_ref[2], base_ref[2], by_columns, preferred_element_type=jnp.float32)
    moves.append(full * (0.01 * scale_ref[0, 2]))
    blocks = base_ref.shape[1] // block
    for j in range(blocks):
        owner = step * blocks + j
        place = (owner - me) % SIDE
        away = owner // SIDE ^ me // SIDE
        for t, (near, far) in enumerate(TURNS):

            @pl.when(place // 2 == t)
            def _(t=t, near=near, far=far):
                for sources, mask in zip(held[t], (0, near, far, near ^ far)):

                    @pl.when(away == mask)
                    def _(sources=sources):
                        if isinstance(sources, tuple):
                            old_ref[...] = jnp.where(place % 2 == 0, sources[0][0], sources[1][0])
                        else:
                            old_ref[...] = sources[place % 2]

        old = old_ref[...].astype(jnp.float32)
        near = slice(j * block, (j + 1) * block)
        copy_forget[near] = (old[:block] - moves[0][near]).astype(jnp.bfloat16)
        copy_value[near] = (old[block : 2 * block] - moves[1][near]).astype(jnp.bfloat16)
        across = slice(j * width, (j + 1) * width)
        for h in range(outw_ref.shape[0] // block):
            down = slice(h * block, (h + 1) * block)
            piece = old[2 * block :, h * width : (h + 1) * width]
            copy_out[down, across] = (piece - moves[2][down, across]).astype(jnp.bfloat16)


def finish(me, sums, arrived, bases, forget_weight, value_weight, out_weight, held, entries, steps=4):
    block, columns = forget_weight.shape
    model, rank = bases.shape[1:]
    tile = model // steps
    whole = lambda a: pl.BlockSpec(a.shape, lambda i, me: (0,) * a.ndim)
    old = (forget_weight, value_weight, out_weight)
    own = [jax.ShapeDtypeStruct(a.shape, jnp.float32) for a in old]
    copies = [jax.ShapeDtypeStruct((model, columns), jnp.bfloat16)] * 2
    copies.append(jax.ShapeDtypeStruct((out_weight.shape[0], model), jnp.bfloat16))
    down = pl.BlockSpec((tile, columns), lambda i, me: (i, 0))
    across = pl.BlockSpec((out_weight.shape[0], tile), lambda i, me: (0, i))
    flat = [a for stream in held for a in stream]
    return pl.pallas_call(
        functools.partial(finish_kernel, entries),
        grid_spec=pltpu.PrefetchScalarGridSpec(
            num_scalar_prefetch=1,
            grid=(steps,),
            in_specs=[
                whole(sums),
                whole(arrived),
                pl.BlockSpec((3, tile, rank), lambda i, me: (0, i, 0)),
                pl.BlockSpec((3, block, rank), lambda i, me: (0, me[0], 0)),
                *map(whole, old),
                *map(whole, flat),
            ],
            out_specs=[
                *map(whole, own),
                down,
                down,
                across,
                *map(whole, own),
            ],
            scratch_shapes=[
                pltpu.VMEM((3, rank, columns), jnp.bfloat16),
                pltpu.VMEM((1, 128), jnp.float32),
                pltpu.VMEM(flat[0].shape[1:], flat[0].dtype),
            ],
        ),
        out_shape=(*own, *copies, *own),
        compiler_params=LARGE,
        name="finish",
    )(me[None], sums, arrived, *[pltpu.with_memory_space_constraint(a, pltpu.HBM) for a in (bases, bases, *old)], *flat)


def along(value, away):
    pairs = [(i, i // SIDE * SIDE + (i - away) % SIDE) for i in range(lax.axis_size(FS))]
    return lax.ppermute(value, FS, pairs)


def passed(value, mask):
    return lax.ppermute(value, FS, [(i, i ^ mask * SIDE) for i in range(lax.axis_size(FS))])


def join_kernel(own_ref, one_ref, two_ref, three_ref, low_ref, high_ref):
    low_ref[0] = own_ref[0]
    low_ref[1] = one_ref[0]
    high_ref[0] = two_ref[0]
    high_ref[1] = three_ref[0]


def joined(*blocks):
    shape, dtype = blocks[0].shape, blocks[0].dtype
    pair = jax.ShapeDtypeStruct((2, *shape[1:]), dtype)
    return pl.pallas_call(
        join_kernel, out_shape=(pair, pair), compiler_params=SMALL, name="join"
    )(*blocks)


def on_device(
    normed_input,
    forget_cot,
    value_cot,
    gated_output,
    output_cot,
    forget_weight,
    value_weight,
    out_weight,
    bases,
    first_moment,
    second_moment,
):
    owners = lax.axis_size(FS)
    me = lax.axis_index(FS).astype(jnp.int32)
    factor = float(normed_input.shape[0] * owners) ** (-0.5)
    rank, columns = bases.shape[2], forget_cot.shape[1]
    packed = pack(opening(), forget_weight, value_weight, out_weight)
    one, three, two = (along(packed, away) for away in (1, 3, 2))
    at_near, at_far = (passed(packed, mask) for mask in (NEAR, FAR))
    inputs = (normed_input, normed_input, output_cot)
    cots = (forget_cot, value_cot, gated_output)
    reduced = [reduced_part(x, bases[k]) for k, x in enumerate(inputs)]
    reduced = lax.optimization_barrier(tuple(reduced))
    parts = [projected_part(r, c, factor) for r, c in zip(reduced, cots)]
    part = jnp.stack([p.reshape(owners, rank // owners, columns) for p in parts], axis=1)
    held = joined(packed, one, two, three)
    part, *held = lax.optimization_barrier((part, *held))
    arrived = lax.all_to_all(part, FS, split_axis=0, concat_axis=0, tiled=True)
    nearer = [passed(a, near) for a, (near, _) in zip(held, TURNS)]
    far_one, near_three = along(at_far, 1), along(at_near, 3)
    moment_one, moment_two, messages = moments(
        arrived, jnp.moveaxis(first_moment, 1, 0), jnp.moveaxis(second_moment, 1, 0)
    )
    gathered = lax.all_to_all(messages, FS, split_axis=0, concat_axis=0, tiled=True)
    across = [passed(a, far) for a, (_, far) in zip(nearer, TURNS)]
    near_two = along(near_three, 3)
    sums = squares(gathered, lax.axis_size(TP))
    sums = lax.all_to_all(sums, TP, split_axis=0, concat_axis=0, tiled=True)
    entries = float(rank * columns * lax.axis_size(TP))
    finished = finish(
        me,
        sums,
        gathered,
        bases,
        forget_weight,
        value_weight,
        out_weight,
        list(zip(held, nearer, (at_far, near_two), (far_one, near_three), across)),
        entries,
    )
    moment_one, moment_two = (jnp.moveaxis(m, 0, 1) for m in (moment_one, moment_two))
    return (*finished[:6], moment_one, moment_two, *finished[6:])


def solution(mesh):
    torus = Mesh(mesh.devices.reshape(4, 4, 4, 2), ("fs_0", "fs_1", "tp_0", "tp_1"))
    placed = (
        P(FS, None),
        P(FS, TP),
        P(FS, TP),
        P(FS, TP),
        P(FS, None),
        P(FS, TP),
        P(FS, TP),
        P(TP, FS),
        P(),
        P(FS, None, TP),
        P(FS, None, TP),
    )
    return jax.shard_map(
        on_device,
        mesh=torus,
        in_specs=placed,
        out_specs=(
            P(FS, TP),
            P(FS, TP),
            P(TP, FS),
            P(None, TP),
            P(None, TP),
            P(TP, None),
            P(FS, None, TP),
            P(FS, None, TP),
            P(FS, TP),
            P(FS, TP),
            P(TP, FS),
        ),
        check_vma=False,
    )
```

```python
import functools

import jax
import jax.numpy as jnp
from jax import lax
from jax.experimental import pallas as pl
from jax.experimental.pallas import tpu as pltpu
from jax.sharding import Mesh
from jax.sharding import PartitionSpec as P


FS = ("fs_0", "fs_1")
TP = ("tp_0", "tp_1")

NEAR, FAR = 1, 3
SIDE = 4
TURNS = ((NEAR, FAR), (FAR, NEAR))
EARLY = pl.CostEstimate(flops=1 << 34, bytes_accessed=1 << 20, transcendentals=0)
SMALL = pltpu.CompilerParams(vmem_limit_bytes=8 << 20)
LARGE = pltpu.CompilerParams(vmem_limit_bytes=24 << 20)


def opening_kernel(out_ref):
    out_ref[...] = jnp.zeros_like(out_ref)


def opening():
    return pl.pallas_call(
        opening_kernel,
        out_shape=jax.ShapeDtypeStruct((8, 128), jnp.float32),
        cost_estimate=EARLY,
        compiler_params=SMALL,
        name="opening",
    )()


def pack_kernel(_, forget_ref, value_ref, out_ref, packed_ref):
    rows = forget_ref.shape[0]
    width = out_ref.shape[1]
    packed_ref[0, :rows] = forget_ref[...].astype(jnp.bfloat16)
    packed_ref[0, rows : 2 * rows] = value_ref[...].astype(jnp.bfloat16)
    for h in range(out_ref.shape[0] // rows):
        part = out_ref[pl.ds(h * rows, rows)]
        packed_ref[0, 2 * rows :, h * width : (h + 1) * width] = part.astype(jnp.bfloat16)


def pack(opened, *weights):
    rows, columns = weights[0].shape
    return pl.pallas_call(
        pack_kernel,
        out_shape=jax.ShapeDtypeStruct((1, 3 * rows, columns), jnp.bfloat16),
        cost_estimate=EARLY,
        compiler_params=SMALL,
        name="pack",
    )(opened, *weights)


def reduced_part(x, basis):
    reduced = lax.dot_general(
        basis, x, (((0,), (1,)), ((), ())), preferred_element_type=jnp.float32
    )
    return reduced.astype(jnp.bfloat16)


def projected_part(reduced, cot, factor):
    part = jnp.dot(reduced, cot, preferred_element_type=jnp.float32)
    return (part * factor).astype(jnp.bfloat16)


def moment_kernel(arrived_ref, first_ref, second_ref, one_ref, two_ref, message_ref):
    rows = first_ref.shape[1]
    for k in range(3):
        projected = jnp.sum(arrived_ref[:, k].astype(jnp.float32), axis=0)
        one = 0.9 * first_ref[k] + 0.1 * projected
        two = 0.9 * second_ref[k] + 0.1 * projected * projected
        one_ref[k] = one
        two_ref[k] = two
        direction = (one / (jnp.sqrt(two) + 1e-08)).astype(jnp.bfloat16)
        for i in range(message_ref.shape[0]):
            message_ref[i, k * rows : (k + 1) * rows] = direction


def moments(arrived, first_moment, second_moment):
    _, rows, columns = first_moment.shape
    moment = jax.ShapeDtypeStruct(first_moment.shape, jnp.float32)
    messages = pltpu.HBM((arrived.shape[0], 3 * rows, columns), jnp.bfloat16)
    return pl.pallas_call(
        moment_kernel,
        out_shape=(moment, moment, messages),
        compiler_params=SMALL,
        name="moments",
    )(arrived, first_moment, second_moment)


def square_kernel(arrived_ref, sum_ref):
    rows = arrived_ref.shape[1] // 3
    lane = lax.broadcasted_iota(jnp.int32, sum_ref.shape, 2)
    sums = jnp.zeros(sum_ref.shape, jnp.float32)
    for k in range(3):
        direction = arrived_ref[:, k * rows : (k + 1) * rows].astype(jnp.float32)
        sums = jnp.where(lane == k, jnp.sum(direction * direction), sums)
    sum_ref[...] = sums


def squares(arrived, copies):
    return pl.pallas_call(
        square_kernel,
        out_shape=jax.ShapeDtypeStruct((copies, 1, 128), jnp.float32),
        compiler_params=SMALL,
        name="squares",
    )(arrived)


def finish_kernel(entries, me_ref, sums_ref, arrived_ref, base_ref, mine_ref, forget_ref, value_ref, outw_ref, *refs):
    streams = len(TURNS)
    held = []
    for t in range(streams):
        whole, nearer, even, odd, across = refs[5 * t : 5 * t + 5]
        held.append((whole, nearer, (even, odd), across))
    (
        new_forget,
        new_value,
        new_out,
        copy_forget,
        copy_value,
        copy_out,
        step_forget,
        step_value,
        step_out,
        dir_ref,
        scale_ref,
        old_ref,
    ) = refs[5 * streams :]
    step = pl.program_id(0)
    owners = arrived_ref.shape[0]
    rank = dir_ref.shape[1]
    rows = rank // owners
    block = mine_ref.shape[1]
    width = outw_ref.shape[1]
    me = me_ref[0]
    by_columns = (((1,), (1,)), ((), ()))

    @pl.when(step == 0)
    def _():
        sums = jnp.sum(sums_ref[...], axis=0)
        scale_ref[...] = lax.rsqrt(sums / entries + 1.0)
        for k in range(3):
            direction = arrived_ref[:, k * rows : (k + 1) * rows, :].reshape(rank, -1)
            dir_ref[k] = direction if k < 2 else direction.T
        for k, (old, new, moved) in enumerate(
            ((forget_ref, new_forget, step_forget), (value_ref, new_value, step_value))
        ):
            full = jnp.dot(mine_ref[k], dir_ref[k], preferred_element_type=jnp.float32)
            full = full * scale_ref[0, k]
            moved[...] = full
            new[...] = old[...] - 0.01 * full
        full = lax.dot_general(dir_ref[2], mine_ref[2], by_columns, preferred_element_type=jnp.float32)
        full = full * scale_ref[0, 2]
        step_out[...] = full
        new_out[...] = outw_ref[...] - 0.01 * full

    moves = []
    for k in range(2):
        full = jnp.dot(base_ref[k], dir_ref[k], preferred_element_type=jnp.float32)
        moves.append(full * (0.01 * scale_ref[0, k]))
    full = lax.dot_general(dir_ref[2], base_ref[2], by_columns, preferred_element_type=jnp.float32)
    moves.append(full * (0.01 * scale_ref[0, 2]))
    blocks = base_ref.shape[1] // block
    for j in range(blocks):
        owner = step * blocks + j
        place = (owner - me) % SIDE
        away = owner // SIDE ^ me // SIDE
        for t, (near, far) in enumerate(TURNS):

            @pl.when(place // 2 == t)
            def _(t=t, near=near, far=far):
                for sources, mask in zip(held[t], (0, near, far, near ^ far)):

                    @pl.when(away == mask)
                    def _(sources=sources):
                        if isinstance(sources, tuple):
                            old_ref[...] = jnp.where(place % 2 == 0, sources[0][0], sources[1][0])
                        else:
                            old_ref[...] = sources[place % 2]

        old = old_ref[...].astype(jnp.float32)
        near = slice(j * block, (j + 1) * block)
        copy_forget[near] = (old[:block] - moves[0][near]).astype(jnp.bfloat16)
        copy_value[near] = (old[block : 2 * block] - moves[1][near]).astype(jnp.bfloat16)
        across = slice(j * width, (j + 1) * width)
        for h in range(outw_ref.shape[0] // block):
            down = slice(h * block, (h + 1) * block)
            piece = old[2 * block :, h * width : (h + 1) * width]
            copy_out[down, across] = (piece - moves[2][down, across]).astype(jnp.bfloat16)


def finish(me, sums, arrived, bases, forget_weight, value_weight, out_weight, held, entries, steps=2):
    block, columns = forget_weight.shape
    model, rank = bases.shape[1:]
    tile = model // steps
    whole = lambda a: pl.BlockSpec(a.shape, lambda i, me: (0,) * a.ndim)
    old = (forget_weight, value_weight, out_weight)
    own = [jax.ShapeDtypeStruct(a.shape, jnp.float32) for a in old]
    copies = [jax.ShapeDtypeStruct((model, columns), jnp.bfloat16)] * 2
    copies.append(jax.ShapeDtypeStruct((out_weight.shape[0], model), jnp.bfloat16))
    down = pl.BlockSpec((tile, columns), lambda i, me: (i, 0))
    across = pl.BlockSpec((out_weight.shape[0], tile), lambda i, me: (0, i))
    flat = [a for stream in held for a in stream]
    return pl.pallas_call(
        functools.partial(finish_kernel, entries),
        grid_spec=pltpu.PrefetchScalarGridSpec(
            num_scalar_prefetch=1,
            grid=(steps,),
            in_specs=[
                whole(sums),
                whole(arrived),
                pl.BlockSpec((3, tile, rank), lambda i, me: (0, i, 0)),
                pl.BlockSpec((3, block, rank), lambda i, me: (0, me[0], 0)),
                *map(whole, old),
                *map(whole, flat),
            ],
            out_specs=[
                *map(whole, own),
                down,
                down,
                across,
                *map(whole, own),
            ],
            scratch_shapes=[
                pltpu.VMEM((3, rank, columns), jnp.bfloat16),
                pltpu.VMEM((1, 128), jnp.float32),
                pltpu.VMEM(flat[0].shape[1:], flat[0].dtype),
            ],
        ),
        out_shape=(*own, *copies, *own),
        compiler_params=LARGE,
        name="finish",
    )(me[None], sums, arrived, *[pltpu.with_memory_space_constraint(a, pltpu.HBM) for a in (bases, bases, *old)], *flat)


def along(value, away):
    pairs = [(i, i // SIDE * SIDE + (i - away) % SIDE) for i in range(lax.axis_size(FS))]
    return lax.ppermute(value, FS, pairs)


def passed(value, mask):
    return lax.ppermute(value, FS, [(i, i ^ mask * SIDE) for i in range(lax.axis_size(FS))])


def join_kernel(own_ref, one_ref, two_ref, three_ref, low_ref, high_ref):
    low_ref[0] = own_ref[0]
    low_ref[1] = one_ref[0]
    high_ref[0] = two_ref[0]
    high_ref[1] = three_ref[0]


def joined(*blocks):
    shape, dtype = blocks[0].shape, blocks[0].dtype
    pair = jax.ShapeDtypeStruct((2, *shape[1:]), dtype)
    return pl.pallas_call(
        join_kernel, out_shape=(pair, pair), compiler_params=SMALL, name="join"
    )(*blocks)


def on_device(
    normed_input,
    forget_cot,
    value_cot,
    gated_output,
    output_cot,
    forget_weight,
    value_weight,
    out_weight,
    bases,
    first_moment,
    second_moment,
):
    owners = lax.axis_size(FS)
    me = lax.axis_index(FS).astype(jnp.int32)
    factor = float(normed_input.shape[0] * owners) ** (-0.5)
    rank, columns = bases.shape[2], forget_cot.shape[1]
    packed = pack(opening(), forget_weight, value_weight, out_weight)
    one, three, two = (along(packed, away) for away in (1, 3, 2))
    at_near, at_far = (passed(packed, mask) for mask in (NEAR, FAR))
    inputs = (normed_input, normed_input, output_cot)
    cots = (forget_cot, value_cot, gated_output)
    parts = []
    for k, (x, cot) in enumerate(zip(inputs, cots)):
        x, parts = lax.optimization_barrier((x, parts))
        reduced = reduced_part(x, bases[k])
        parts.append(projected_part(lax.optimization_barrier(reduced), cot, factor))
    part = jnp.stack([p.reshape(owners, rank // owners, columns) for p in parts], axis=1)
    held = joined(packed, one, two, three)
    part, *held = lax.optimization_barrier((part, *held))
    arrived = lax.all_to_all(part, FS, split_axis=0, concat_axis=0, tiled=True)
    nearer = [passed(a, near) for a, (near, _) in zip(held, TURNS)]
    far_one, near_three = along(at_far, 1), along(at_near, 3)
    moment_one, moment_two, messages = moments(
        arrived, jnp.moveaxis(first_moment, 1, 0), jnp.moveaxis(second_moment, 1, 0)
    )
    gathered = lax.all_to_all(messages, FS, split_axis=0, concat_axis=0, tiled=True)
    across = [passed(a, far) for a, (_, far) in zip(nearer, TURNS)]
    near_two = along(near_three, 3)
    sums = squares(gathered, lax.axis_size(TP))
    sums = lax.all_to_all(sums, TP, split_axis=0, concat_axis=0, tiled=True)
    entries = float(rank * columns * lax.axis_size(TP))
    finished = finish(
        me,
        sums,
        gathered,
        bases,
        forget_weight,
        value_weight,
        out_weight,
        list(zip(held, nearer, (at_far, near_two), (far_one, near_three), across)),
        entries,
    )
    moment_one, moment_two = (jnp.moveaxis(m, 0, 1) for m in (moment_one, moment_two))
    return (*finished[:6], moment_one, moment_two, *finished[6:])


def solution(mesh):
    torus = Mesh(mesh.devices.reshape(4, 4, 4, 2), ("fs_0", "fs_1", "tp_0", "tp_1"))
    placed = (
        P(FS, None),
        P(FS, TP),
        P(FS, TP),
        P(FS, TP),
        P(FS, None),
        P(FS, TP),
        P(FS, TP),
        P(TP, FS),
        P(),
        P(FS, None, TP),
        P(FS, None, TP),
    )
    return jax.shard_map(
        on_device,
        mesh=torus,
        in_specs=placed,
        out_specs=(
            P(FS, TP),
            P(FS, TP),
            P(TP, FS),
            P(None, TP),
            P(None, TP),
            P(TP, None),
            P(FS, None, TP),
            P(FS, None, TP),
            P(FS, TP),
            P(FS, TP),
            P(TP, FS),
        ),
        check_vma=False,
    )
```

```python
import functools

import jax
import jax.numpy as jnp
from jax import lax
from jax.experimental import pallas as pl
from jax.experimental.pallas import tpu as pltpu
from jax.sharding import Mesh
from jax.sharding import PartitionSpec as P


FS = ("fs_0", "fs_1")
TP = ("tp_0", "tp_1")

NEAR, FAR = 1, 3
SIDE = 4
TURNS = ((NEAR, FAR), (FAR, NEAR))
EARLY = pl.CostEstimate(flops=1 << 34, bytes_accessed=1 << 20, transcendentals=0)
SMALL = pltpu.CompilerParams(vmem_limit_bytes=8 << 20)
LARGE = pltpu.CompilerParams(vmem_limit_bytes=24 << 20)


def opening_kernel(out_ref):
    out_ref[...] = jnp.zeros_like(out_ref)


def opening():
    return pl.pallas_call(
        opening_kernel,
        out_shape=jax.ShapeDtypeStruct((8, 128), jnp.float32),
        cost_estimate=EARLY,
        compiler_params=SMALL,
        name="opening",
    )()


def pack_kernel(_, forget_ref, value_ref, out_ref, packed_ref):
    rows = forget_ref.shape[0]
    width = out_ref.shape[1]
    packed_ref[0, :rows] = forget_ref[...].astype(jnp.bfloat16)
    packed_ref[0, rows : 2 * rows] = value_ref[...].astype(jnp.bfloat16)
    for h in range(out_ref.shape[0] // rows):
        part = out_ref[pl.ds(h * rows, rows)]
        packed_ref[0, 2 * rows :, h * width : (h + 1) * width] = part.astype(jnp.bfloat16)


def pack(opened, *weights):
    rows, columns = weights[0].shape
    return pl.pallas_call(
        pack_kernel,
        out_shape=jax.ShapeDtypeStruct((1, 3 * rows, columns), jnp.bfloat16),
        cost_estimate=EARLY,
        compiler_params=SMALL,
        name="pack",
    )(opened, *weights)


def reduced_part(x, basis):
    reduced = lax.dot_general(
        basis, x, (((0,), (1,)), ((), ())), preferred_element_type=jnp.float32
    )
    return reduced.astype(jnp.bfloat16)


def projected_part(reduced, cot, factor):
    part = jnp.dot(reduced, cot, preferred_element_type=jnp.float32)
    return (part * factor).astype(jnp.bfloat16)


def moment_kernel(arrived_ref, first_ref, second_ref, one_ref, two_ref, message_ref):
    rows = first_ref.shape[1]
    for k in range(3):
        projected = jnp.sum(arrived_ref[:, k].astype(jnp.float32), axis=0)
        one = 0.9 * first_ref[k] + 0.1 * projected
        two = 0.9 * second_ref[k] + 0.1 * projected * projected
        one_ref[k] = one
        two_ref[k] = two
        direction = (one / (jnp.sqrt(two) + 1e-08)).astype(jnp.bfloat16)
        for i in range(message_ref.shape[0]):
            message_ref[i, k * rows : (k + 1) * rows] = direction


def moments(arrived, first_moment, second_moment):
    _, rows, columns = first_moment.shape
    moment = jax.ShapeDtypeStruct(first_moment.shape, jnp.float32)
    messages = pltpu.HBM((arrived.shape[0], 3 * rows, columns), jnp.bfloat16)
    return pl.pallas_call(
        moment_kernel,
        out_shape=(moment, moment, messages),
        compiler_params=SMALL,
        name="moments",
    )(arrived, first_moment, second_moment)


def square_kernel(arrived_ref, sum_ref):
    rows = arrived_ref.shape[1] // 3
    lane = lax.broadcasted_iota(jnp.int32, sum_ref.shape, 2)
    sums = jnp.zeros(sum_ref.shape, jnp.float32)
    for k in range(3):
        direction = arrived_ref[:, k * rows : (k + 1) * rows].astype(jnp.float32)
        sums = jnp.where(lane == k, jnp.sum(direction * direction), sums)
    sum_ref[...] = sums


def squares(arrived, copies):
    return pl.pallas_call(
        square_kernel,
        out_shape=jax.ShapeDtypeStruct((copies, 1, 128), jnp.float32),
        compiler_params=SMALL,
        name="squares",
    )(arrived)


def finish_kernel(entries, me_ref, sums_ref, arrived_ref, base_ref, mine_ref, forget_ref, value_ref, outw_ref, *refs):
    streams = len(TURNS)
    held = []
    for t in range(streams):
        whole, nearer, even, odd, across = refs[5 * t : 5 * t + 5]
        held.append((whole, nearer, (even, odd), across))
    (
        new_forget,
        new_value,
        new_out,
        copy_forget,
        copy_value,
        copy_out,
        step_forget,
        step_value,
        step_out,
        dir_ref,
        scale_ref,
        old_ref,
    ) = refs[5 * streams :]
    step = pl.program_id(0)
    owners = arrived_ref.shape[0]
    rank = dir_ref.shape[1]
    rows = rank // owners
    block = mine_ref.shape[1]
    width = outw_ref.shape[1]
    me = me_ref[0]
    by_columns = (((1,), (1,)), ((), ()))

    @pl.when(step == 0)
    def _():
        sums = jnp.sum(sums_ref[...], axis=0)
        scale_ref[...] = lax.rsqrt(sums / entries + 1.0)
        for k in range(3):
            direction = arrived_ref[:, k * rows : (k + 1) * rows, :].reshape(rank, -1)
            dir_ref[k] = direction if k < 2 else direction.T
        for k, (old, new, moved) in enumerate(
            ((forget_ref, new_forget, step_forget), (value_ref, new_value, step_value))
        ):
            full = jnp.dot(mine_ref[k], dir_ref[k], preferred_element_type=jnp.float32)
            full = full * scale_ref[0, k]
            moved[...] = full
            new[...] = old[...] - 0.01 * full
        full = lax.dot_general(dir_ref[2], mine_ref[2], by_columns, preferred_element_type=jnp.float32)
        full = full * scale_ref[0, 2]
        step_out[...] = full
        new_out[...] = outw_ref[...] - 0.01 * full

    moves = []
    for k in range(2):
        full = jnp.dot(base_ref[k], dir_ref[k], preferred_element_type=jnp.float32)
        moves.append(full * (0.01 * scale_ref[0, k]))
    full = lax.dot_general(dir_ref[2], base_ref[2], by_columns, preferred_element_type=jnp.float32)
    moves.append(full * (0.01 * scale_ref[0, 2]))
    blocks = base_ref.shape[1] // block
    rows_here = blocks // SIDE
    for j in range(rows_here):
        away = (step * rows_here + j) ^ (me // SIDE)
        for t, (near, far) in enumerate(TURNS):
            for sources, mask in zip(held[t], (0, near, far, near ^ far)):

                @pl.when(away == mask)
                def _(sources=sources, t=t, j=j):
                    for n in range(2):
                        owner = j * SIDE + (me + 2 * t + n) % SIDE
                        old_ref[owner] = sources[n][0] if isinstance(sources, tuple) else sources[n]

    for j in range(blocks):
        old = old_ref[j].astype(jnp.float32)
        near = slice(j * block, (j + 1) * block)
        copy_forget[near] = (old[:block] - moves[0][near]).astype(jnp.bfloat16)
        copy_value[near] = (old[block : 2 * block] - moves[1][near]).astype(jnp.bfloat16)
        across = slice(j * width, (j + 1) * width)
        for h in range(outw_ref.shape[0] // block):
            down = slice(h * block, (h + 1) * block)
            piece = old[2 * block :, h * width : (h + 1) * width]
            copy_out[down, across] = (piece - moves[2][down, across]).astype(jnp.bfloat16)


def finish(me, sums, arrived, bases, forget_weight, value_weight, out_weight, held, entries, steps=2):
    block, columns = forget_weight.shape
    model, rank = bases.shape[1:]
    tile = model // steps
    whole = lambda a: pl.BlockSpec(a.shape, lambda i, me: (0,) * a.ndim)
    old = (forget_weight, value_weight, out_weight)
    own = [jax.ShapeDtypeStruct(a.shape, jnp.float32) for a in old]
    copies = [jax.ShapeDtypeStruct((model, columns), jnp.bfloat16)] * 2
    copies.append(jax.ShapeDtypeStruct((out_weight.shape[0], model), jnp.bfloat16))
    down = pl.BlockSpec((tile, columns), lambda i, me: (i, 0))
    across = pl.BlockSpec((out_weight.shape[0], tile), lambda i, me: (0, i))
    flat = [a for stream in held for a in stream]
    return pl.pallas_call(
        functools.partial(finish_kernel, entries),
        grid_spec=pltpu.PrefetchScalarGridSpec(
            num_scalar_prefetch=1,
            grid=(steps,),
            in_specs=[
                whole(sums),
                whole(arrived),
                pl.BlockSpec((3, tile, rank), lambda i, me: (0, i, 0)),
                pl.BlockSpec((3, block, rank), lambda i, me: (0, me[0], 0)),
                *map(whole, old),
                *map(whole, flat),
            ],
            out_specs=[
                *map(whole, own),
                down,
                down,
                across,
                *map(whole, own),
            ],
            scratch_shapes=[
                pltpu.VMEM((3, rank, columns), jnp.bfloat16),
                pltpu.VMEM((1, 128), jnp.float32),
                pltpu.VMEM((tile // block, *flat[0].shape[1:]), flat[0].dtype),
            ],
        ),
        out_shape=(*own, *copies, *own),
        compiler_params=LARGE,
        name="finish",
    )(me[None], sums, arrived, *[pltpu.with_memory_space_constraint(a, pltpu.HBM) for a in (bases, bases, *old)], *flat)


def along(value, away):
    pairs = [(i, i // SIDE * SIDE + (i - away) % SIDE) for i in range(lax.axis_size(FS))]
    return lax.ppermute(value, FS, pairs)


def passed(value, mask):
    return lax.ppermute(value, FS, [(i, i ^ mask * SIDE) for i in range(lax.axis_size(FS))])


def join_kernel(own_ref, one_ref, two_ref, three_ref, low_ref, high_ref):
    low_ref[0] = own_ref[0]
    low_ref[1] = one_ref[0]
    high_ref[0] = two_ref[0]
    high_ref[1] = three_ref[0]


def joined(*blocks):
    shape, dtype = blocks[0].shape, blocks[0].dtype
    pair = jax.ShapeDtypeStruct((2, *shape[1:]), dtype)
    return pl.pallas_call(
        join_kernel, out_shape=(pair, pair), compiler_params=SMALL, name="join"
    )(*blocks)


def on_device(
    normed_input,
    forget_cot,
    value_cot,
    gated_output,
    output_cot,
    forget_weight,
    value_weight,
    out_weight,
    bases,
    first_moment,
    second_moment,
):
    owners = lax.axis_size(FS)
    me = lax.axis_index(FS).astype(jnp.int32)
    factor = float(normed_input.shape[0] * owners) ** (-0.5)
    rank, columns = bases.shape[2], forget_cot.shape[1]
    packed = pack(opening(), forget_weight, value_weight, out_weight)
    one, three, two = (along(packed, away) for away in (1, 3, 2))
    at_near, at_far = (passed(packed, mask) for mask in (NEAR, FAR))
    inputs = (normed_input, normed_input, output_cot)
    cots = (forget_cot, value_cot, gated_output)
    parts = []
    for k, (x, cot) in enumerate(zip(inputs, cots)):
        x, parts = lax.optimization_barrier((x, parts))
        reduced = reduced_part(x, bases[k])
        parts.append(projected_part(lax.optimization_barrier(reduced), cot, factor))
    part = jnp.stack([p.reshape(owners, rank // owners, columns) for p in parts], axis=1)
    held = joined(packed, one, two, three)
    part, *held = lax.optimization_barrier((part, *held))
    arrived = lax.all_to_all(part, FS, split_axis=0, concat_axis=0, tiled=True)
    nearer = [passed(a, near) for a, (near, _) in zip(held, TURNS)]
    moment_one, moment_two, messages = moments(
        arrived, jnp.moveaxis(first_moment, 1, 0), jnp.moveaxis(second_moment, 1, 0)
    )
    gathered = lax.all_to_all(messages, FS, split_axis=0, concat_axis=0, tiled=True)
    far_one = along(at_far, 1)
    near_two, near_three = along(at_near, 2), along(at_near, 3)
    across = [passed(a, far) for a, (_, far) in zip(nearer, TURNS)]
    sums = squares(gathered, lax.axis_size(TP))
    sums = lax.all_to_all(sums, TP, split_axis=0, concat_axis=0, tiled=True)
    entries = float(rank * columns * lax.axis_size(TP))
    finished = finish(
        me,
        sums,
        gathered,
        bases,
        forget_weight,
        value_weight,
        out_weight,
        list(zip(held, nearer, (at_far, near_two), (far_one, near_three), across)),
        entries,
    )
    moment_one, moment_two = (jnp.moveaxis(m, 0, 1) for m in (moment_one, moment_two))
    return (*finished[:6], moment_one, moment_two, *finished[6:])


def solution(mesh):
    torus = Mesh(mesh.devices.reshape(4, 4, 4, 2), ("fs_0", "fs_1", "tp_0", "tp_1"))
    placed = (
        P(FS, None),
        P(FS, TP),
        P(FS, TP),
        P(FS, TP),
        P(FS, None),
        P(FS, TP),
        P(FS, TP),
        P(TP, FS),
        P(),
        P(FS, None, TP),
        P(FS, None, TP),
    )
    return jax.shard_map(
        on_device,
        mesh=torus,
        in_specs=placed,
        out_specs=(
            P(FS, TP),
            P(FS, TP),
            P(TP, FS),
            P(None, TP),
            P(None, TP),
            P(TP, None),
            P(FS, None, TP),
            P(FS, None, TP),
            P(FS, TP),
            P(FS, TP),
            P(TP, FS),
        ),
        check_vma=False,
    )
```
